32 devices in a mesh: ep: 32 (over z, y, x, core).
Axes of the slice: x: 2, y: 2, z: 4, core: 2. Of those that a mesh axis runs over, the one named last changes fastest.
Arguments:
- latest_embeddings: bfloat16 [512, 2048], P('ep'), may hold values from -6 to 6
- prior_memory_grids: float32 [512, 32, 4096], P('ep'), may hold values from -1.75 to 1.75
- earlier_rescale_gain: float32 [2048], replicated, may hold values from 0.1 to 1.9
- query_map: bfloat16 [2048, 2048], P(None, 'ep'), may hold values from -0.125 to 0.125
- lookup_map: bfloat16 [2048, 2048], P(None, 'ep'), may hold values from -0.125 to 0.125
- content_map: bfloat16 [2048, 2048], P(None, 'ep'), may hold values from -0.125 to 0.125
- forget_lower_map: bfloat16 [2048, 64], replicated, may hold values from -0.125 to 0.125
- forget_upper_map: bfloat16 [64, 2048], replicated, may hold values from -0.75 to 0.75
- forget_shift: float32 [2048], replicated, may hold values from -3 to 3
- adapt_lower_map: bfloat16 [2048, 64], replicated, may hold values from -0.125 to 0.125
- adapt_upper_map: bfloat16 [64, 2048], replicated, may hold values from -0.75 to 0.75
- adapt_shift: float32 [2048], replicated, may hold values from -2 to 2
- erase_lookup_gains: float32 [2048], replicated, may hold values from 0.1 to 1.9
- substitute_lookup_gains: float32 [2048], replicated, may hold values from 0.1 to 1.9
- present_extra_gains: float32 [2048], replicated, may hold values from -1.75 to 1.75
- attender_rescale_gain: float32 [2048], replicated, may hold values from 0.1 to 1.9
- result_map: bfloat16 [2048, 2048], P(None, 'ep'), may hold values from -0.125 to 0.125
- later_rescale_gain: float32 [2048], replicated, may hold values from 0.1 to 1.9
- specialist_switch_maps: bfloat16 [32, 2048, 512], P('ep'), may hold values from -0.125 to 0.125
- specialist_widen_maps: bfloat16 [32, 2048, 512], P('ep'), may hold values from -0.125 to 0.125
- specialist_shrink_maps: bfloat16 [32, 512, 2048], P('ep'), may hold values from -0.25 to 0.25
- picked_specialists: int32 [512, 6], P('ep'), may hold values from 0 to 31, as said below
- specialist_picked_shares: float32 [512, 6], P('ep'), may hold values from 0.02 to 0.5
Outputs:
- new_hidden: bfloat16 [512, 2048], P('ep')
- new_state: float32 [512, 32, 4096], P('ep')
The draws below stay inside these ranges and needn't reach their ends.
Inputs may be any that keep to these rules, and one draw needn't show every extreme that they name: `picked_specialists`: each row names 6 different experts of one group; a group is a run of 8 consecutive expert numbers. The rows of one device use exactly two groups, one of them for half of the device's rows rounded up and the other for the rest. No expert is named by more than 6 rows of one device, and on every device some expert is named by exactly 6.
All inputs are finite; a program needn't handle non-finite values.
Results may differ from the reference program's by a relative error of at most 0.011.
Values may be sent and summed in bfloat16 or wider, within the bound.
A program may use at most 256 MiB of HBM per device.

```python
import math
import jax
import jax.numpy as jnp
from jax import lax

EMBED_WIDTH = 2048
CHANNEL_COUNT = 64
ATTENDER_COUNT = 32
LR = 64
FE = 512
GROUPS = 4
TOP = 6
EXPERTS = 32
SEQ_DEV = 16
SEQS = 512
CAP = 6
N_EP = 32


def draw_picked_specialists(key, part):
    group_size = EXPERTS // GROUPS
    half_rows = (SEQ_DEV + 1) // 2

    def one_device(device):
        base = jax.random.fold_in(jax.random.fold_in(key, 17), device)
        subkeys = jax.random.split(base, 5)
        ranking = jax.random.permutation(subkeys[0], SEQ_DEV)
        first_group = jax.random.randint(subkeys[1], (), 0, GROUPS)
        other_group = (first_group + 1 + jax.random.randint(subkeys[2], (), 0, GROUPS - 1)) % GROUPS
        leading = ranking < half_rows
        group_ids = jnp.where(leading, first_group, other_group)
        within_group = jnp.where(leading, ranking, ranking - half_rows)
        order_first = jax.random.permutation(subkeys[3], group_size)
        order_other = jax.random.permutation(subkeys[4], group_size)
        positions = (within_group[:, None] * TOP + jnp.arange(TOP)[None, :]) % group_size
        chosen = jnp.where(leading[:, None], order_first[positions], order_other[positions])
        return (group_ids[:, None] * group_size + chosen).astype(jnp.int32)
    blocks = jax.vmap(one_device)(jnp.arange(N_EP))
    return blocks.reshape(SEQ_DEV * N_EP, TOP)


def steps_of(own_key, shape, shards, low, largest):
    level = 1.0
    for axis_at, blocks in shards:
        heights = jax.random.uniform(jax.random.fold_in(jax.random.fold_in(own_key, 6), axis_at), (blocks,), jnp.float32, low / len(shards), largest / len(shards))
        level = level * jnp.repeat(jnp.exp(heights), shape[axis_at] // blocks).reshape((-1,) + (1,) * (len(shape) - 1 - axis_at))
    return level


def bell_draw(own_key, shape, spread, reach, shards=(), kind=jnp.bfloat16):
    drawn = spread * jax.random.normal(own_key, shape, jnp.float32)
    if shards:
        drawn = drawn * steps_of(own_key, shape, shards, -0.22, 0.18)
    return jnp.clip(drawn, -reach, reach).astype(kind)


def setup_inputs(seed: int = 0) -> dict:
    arg_keys = jax.random.split(jax.random.key(seed), 24)
    latest_embeddings = bell_draw(arg_keys[0], (SEQS, EMBED_WIDTH), 1.0, 6.0, ((0, 32),))
    prior_memory_grids = bell_draw(arg_keys[1], (SEQS, ATTENDER_COUNT, CHANNEL_COUNT * CHANNEL_COUNT), 0.3, 1.75, ((0, 32),), jnp.float32)
    earlier_rescale_gain = jnp.clip(1.0 + 0.18 * jax.random.normal(arg_keys[2], (EMBED_WIDTH,), jnp.float32), 0.1, 1.9)
    query_map = bell_draw(arg_keys[3], (EMBED_WIDTH, EMBED_WIDTH), EMBED_WIDTH ** -0.5, 0.125, ((1, 32),))
    lookup_map = bell_draw(arg_keys[4], (EMBED_WIDTH, EMBED_WIDTH), EMBED_WIDTH ** -0.5, 0.125, ((1, 32),))
    content_map = bell_draw(arg_keys[5], (EMBED_WIDTH, EMBED_WIDTH), EMBED_WIDTH ** -0.5, 0.125, ((1, 32),))
    forget_lower_map = bell_draw(arg_keys[6], (EMBED_WIDTH, LR), EMBED_WIDTH ** -0.5, 0.125)
    forget_upper_map = bell_draw(arg_keys[7], (LR, EMBED_WIDTH), LR ** -0.5, 0.75)
    forget_shift = jnp.clip(jax.random.uniform(arg_keys[8], (EMBED_WIDTH,), jnp.float32, -3.0, 3.0), -3.0, 3.0)
    adapt_lower_map = bell_draw(arg_keys[9], (EMBED_WIDTH, LR), EMBED_WIDTH ** -0.5, 0.125)
    adapt_upper_map = bell_draw(arg_keys[10], (LR, EMBED_WIDTH), LR ** -0.5, 0.75)
    adapt_shift = jnp.clip(jax.random.uniform(arg_keys[11], (EMBED_WIDTH,), jnp.float32, -2.0, 2.0), -2.0, 2.0)
    erase_lookup_gains = jnp.clip(1.0 + 0.18 * jax.random.normal(arg_keys[12], (EMBED_WIDTH,), jnp.float32), 0.1, 1.9)
    substitute_lookup_gains = jnp.clip(1.0 + 0.18 * jax.random.normal(arg_keys[13], (EMBED_WIDTH,), jnp.float32), 0.1, 1.9)
    present_extra_gains = bell_draw(arg_keys[14], (EMBED_WIDTH,), 0.3, 1.75, (), jnp.float32)
    attender_rescale_gain = jnp.clip(1.0 + 0.18 * jax.random.normal(arg_keys[15], (EMBED_WIDTH,), jnp.float32), 0.1, 1.9)
    result_map = bell_draw(arg_keys[16], (EMBED_WIDTH, EMBED_WIDTH), EMBED_WIDTH ** -0.5, 0.125, ((1, 32),))
    later_rescale_gain = jnp.clip(1.0 + 0.18 * jax.random.normal(arg_keys[17], (EMBED_WIDTH,), jnp.float32), 0.1, 1.9)
    specialist_switch_maps = bell_draw(arg_keys[18], (EXPERTS, EMBED_WIDTH, FE), EMBED_WIDTH ** -0.5, 0.125, ((0, 32),))
    specialist_widen_maps = bell_draw(arg_keys[19], (EXPERTS, EMBED_WIDTH, FE), EMBED_WIDTH ** -0.5, 0.125, ((0, 32),))
    specialist_shrink_maps = bell_draw(arg_keys[20], (EXPERTS, FE, EMBED_WIDTH), FE ** -0.5, 0.25, ((0, 32),))
    picked_specialists = draw_picked_specialists(jax.random.fold_in(arg_keys[23], 71), 0)
    specialist_picked_shares = jnp.clip(jnp.exp(math.log(0.5) - 3.218876 * jax.random.uniform(arg_keys[22], (SEQS, TOP), jnp.float32) ** steps_of(arg_keys[22], (SEQS, TOP), ((0, 32),), -0.2, 0.2)), 0.02, 0.5)
    return dict(latest_embeddings=latest_embeddings, prior_memory_grids=prior_memory_grids, earlier_rescale_gain=earlier_rescale_gain, query_map=query_map, lookup_map=lookup_map, content_map=content_map, forget_lower_map=forget_lower_map, forget_upper_map=forget_upper_map, forget_shift=forget_shift, adapt_lower_map=adapt_lower_map, adapt_upper_map=adapt_upper_map, adapt_shift=adapt_shift, erase_lookup_gains=erase_lookup_gains, substitute_lookup_gains=substitute_lookup_gains, present_extra_gains=present_extra_gains, attender_rescale_gain=attender_rescale_gain, result_map=result_map, later_rescale_gain=later_rescale_gain, specialist_switch_maps=specialist_switch_maps, specialist_widen_maps=specialist_widen_maps, specialist_shrink_maps=specialist_shrink_maps, picked_specialists=picked_specialists, specialist_picked_shares=specialist_picked_shares)


norm_eps = 1e-06
group_eps = 0.00064
unit_eps = 1e-06

def rms_norm(rows_in, gain):
    values = rows_in.astype(jnp.float32)
    scale = lax.rsqrt(lax.optimization_barrier(jnp.mean(values * values, axis=-1, keepdims=True)) + norm_eps)
    return (values * scale * gain.astype(jnp.float32)).astype(jnp.bfloat16)

def memory_readout(query_signal, substitute_lookup, content_signals, forget_multiplier, adapt_speed, erase_signal, memory_grid, attender_rescale_gain, present_extra_gains):
    highest = lax.Precision.HIGHEST
    removed = jnp.einsum('bhij,bhj->bhi', memory_grid, erase_signal, precision=highest)
    memory_grid = memory_grid * forget_multiplier[:, :, None, :] - removed[..., None] * (erase_signal * adapt_speed)[:, :, None, :] + content_signals[..., None] * substitute_lookup[:, :, None, :]
    readout = jnp.einsum('bhij,bhj->bhi', memory_grid, query_signal, precision=highest)
    centered = readout - lax.optimization_barrier(jnp.mean(readout, axis=-1, keepdims=True))
    variance = lax.optimization_barrier(jnp.mean(centered * centered, axis=-1, keepdims=True))
    rescaled_result = centered * lax.rsqrt(variance + group_eps) * attender_rescale_gain
    present_extra = lax.optimization_barrier(jnp.sum(query_signal * substitute_lookup * present_extra_gains, axis=-1, keepdims=True)) * content_signals
    return (rescaled_result + present_extra, memory_grid)

def reference(latest_embeddings, prior_memory_grids, earlier_rescale_gain, query_map, lookup_map, content_map, forget_lower_map, forget_upper_map, forget_shift, adapt_lower_map, adapt_upper_map, adapt_shift, erase_lookup_gains, substitute_lookup_gains, present_extra_gains, attender_rescale_gain, result_map, later_rescale_gain, specialist_switch_maps, specialist_widen_maps, specialist_shrink_maps, picked_specialists, specialist_picked_shares):
    normed = rms_norm(latest_embeddings, earlier_rescale_gain)
    query_signal = jnp.dot(normed, query_map, preferred_element_type=jnp.float32).astype(jnp.bfloat16)
    key_rows = jnp.dot(normed, lookup_map, preferred_element_type=jnp.float32).astype(jnp.bfloat16)
    content_signals = jnp.dot(normed, content_map, preferred_element_type=jnp.float32).astype(jnp.bfloat16)
    decay_low = jnp.tanh(jnp.dot(normed, forget_lower_map, preferred_element_type=jnp.float32)).astype(jnp.bfloat16)
    forget_multiplier = jnp.exp(-math.exp(-0.5) * jax.nn.sigmoid(forget_shift + jnp.dot(decay_low, forget_upper_map, preferred_element_type=jnp.float32)))
    rate_low = jnp.dot(normed, adapt_lower_map, preferred_element_type=jnp.float32).astype(jnp.bfloat16)
    adapt_speed = jax.nn.sigmoid(adapt_shift + jnp.dot(rate_low, adapt_upper_map, preferred_element_type=jnp.float32))
    key_float = key_rows.astype(jnp.float32)
    erase_signal = (key_float * erase_lookup_gains).reshape(SEQS, ATTENDER_COUNT, CHANNEL_COUNT)
    erase_signal = erase_signal * lax.rsqrt(lax.optimization_barrier(jnp.sum(erase_signal * erase_signal, axis=-1, keepdims=True)) + unit_eps)
    substitute_lookup = key_float * (1.0 + (adapt_speed - 1.0) * substitute_lookup_gains)

    def blocked(array):
        return array.reshape(N_EP, SEQ_DEV, ATTENDER_COUNT, CHANNEL_COUNT)

    def one_block(block_entry_signal):
        return memory_readout(*block_entry_signal, attender_rescale_gain.reshape(ATTENDER_COUNT, CHANNEL_COUNT), present_extra_gains.reshape(ATTENDER_COUNT, CHANNEL_COUNT))
    mixed_parts, state_parts = lax.map(one_block, (blocked(query_signal.astype(jnp.float32)), blocked(substitute_lookup), blocked(content_signals.astype(jnp.float32)), blocked(forget_multiplier), blocked(adapt_speed), erase_signal.reshape(N_EP, SEQ_DEV, ATTENDER_COUNT, CHANNEL_COUNT), prior_memory_grids.reshape(N_EP, SEQ_DEV, ATTENDER_COUNT, CHANNEL_COUNT, CHANNEL_COUNT)))
    mixed = mixed_parts.reshape(SEQS, EMBED_WIDTH).astype(jnp.bfloat16)
    new_state = state_parts.reshape(SEQS, ATTENDER_COUNT, CHANNEL_COUNT * CHANNEL_COUNT)
    mixer_out = jnp.dot(mixed, result_map, preferred_element_type=jnp.float32).astype(jnp.bfloat16)
    residual = (latest_embeddings.astype(jnp.float32) + mixer_out.astype(jnp.float32)).astype(jnp.bfloat16)
    second = rms_norm(residual, later_rescale_gain)
    slot_count = N_EP * CAP
    flat_ids = picked_specialists.reshape(-1).astype(jnp.int32)

    def one_expert(block_entry_signal):
        expert_id, gate_w, up_w, down_w = block_entry_signal
        matched = flat_ids == expert_id
        ranking = jnp.argsort(jnp.where(matched, 0, 1).astype(jnp.int32), stable=True)[:slot_count].astype(jnp.int32)
        picked_rows = second[ranking // TOP]
        gate_proj = jnp.dot(picked_rows, gate_w, preferred_element_type=jnp.float32)
        up_proj = jnp.dot(picked_rows, up_w, preferred_element_type=jnp.float32)
        hidden_act = (jax.nn.silu(gate_proj) * up_proj).astype(jnp.bfloat16)
        results = jnp.dot(hidden_act, down_w, preferred_element_type=jnp.float32).astype(jnp.bfloat16)
        return (results, ranking, matched[ranking])
    outputs, rankings, is_valid = lax.map(one_expert, (jnp.arange(EXPERTS, dtype=jnp.int32), specialist_switch_maps, specialist_widen_maps, specialist_shrink_maps))
    coefficient = specialist_picked_shares.reshape(-1)[rankings] * is_valid.astype(specialist_picked_shares.dtype)
    contrib = (coefficient[..., None] * outputs.astype(specialist_picked_shares.dtype)).reshape(-1, EMBED_WIDTH)
    expert_sum = jnp.zeros((SEQS, EMBED_WIDTH), specialist_picked_shares.dtype).at[(rankings // TOP).reshape(-1)].add(contrib)
    new_hidden = (residual.astype(jnp.float32) + expert_sum).astype(jnp.bfloat16)
    return (new_hidden, new_state)
```

```python
import functools
import math

import jax
import jax.numpy as jnp
from jax import lax
from jax.experimental import pallas as pl
from jax.experimental.pallas import tpu as pltpu
from jax.sharding import PartitionSpec as P

GROUPS = 4
MESH = pl.DeviceIdType.MESH

norm_eps = 1e-06
group_eps = 0.00064
unit_eps = 1e-06


def rms_norm(rows_in, gain):
    values = rows_in.astype(jnp.float32)
    scale = lax.rsqrt(jnp.mean(values * values, axis=-1, keepdims=True) + norm_eps)
    return (values * scale * gain).astype(jnp.bfloat16)


def state_kernel(
    q_ref, k_ref, v_ref, dl_ref, al_ref, eg_ref, sg_ref, xg_ref, ag_ref, m_ref,
    mixed_ref, out_ref, sum_ref, spread_ref,
):
    rows, span = q_ref.shape
    repeat = rows // eg_ref.shape[0]
    width = 4 * span
    chunks = m_ref.shape[1] // width
    f32, bf16 = jnp.float32, jnp.bfloat16

    @pl.when(pl.program_id(0) == 0)
    def _():
        shape = sum_ref.shape
        sum_ref[...] = jnp.where(
            lax.broadcasted_iota(jnp.int32, shape, 0) // span
            == lax.broadcasted_iota(jnp.int32, shape, 1),
            1.0, 0.0,
        ).astype(bf16)
        shape = spread_ref.shape
        spread_ref[...] = jnp.where(
            lax.broadcasted_iota(jnp.int32, shape, 1) // span
            == lax.broadcasted_iota(jnp.int32, shape, 0) % span,
            1.0, 0.0,
        ).astype(bf16)

    def gains(ref):
        return jnp.concatenate([ref[...]] * repeat, axis=0)

    def wide(x):
        return jnp.concatenate([x] * 4, axis=1)

    def head_sum(x):
        return jnp.sum(x, axis=-1, keepdims=True)

    q = q_ref[...].astype(f32)
    k = k_ref[...].astype(f32)
    v16 = v_ref[...]
    v = v16.astype(f32)
    decay = jnp.exp(-math.exp(-0.5) * jax.nn.sigmoid(dl_ref[...]))
    rate = jax.nn.sigmoid(al_ref[...])
    erase = k * gains(eg_ref)
    erase = erase * lax.rsqrt(head_sum(erase * erase) + unit_eps)
    repl = k * (1.0 + (rate - 1.0) * gains(sg_ref))
    erase_rate = erase * rate
    erase_w, decay_w, query_w = wide(erase), wide(decay), wide(decay * q)
    removed = jnp.zeros((rows, span), f32)
    kept = jnp.zeros((rows, span), f32)
    for c in range(chunks):
        part = pl.ds(c * width, width)
        m = m_ref[:, part]
        picker = sum_ref[part, :]
        removed += jnp.dot((m * erase_w).astype(bf16), picker, preferred_element_type=f32)
        kept += jnp.dot((m * query_w).astype(bf16), picker, preferred_element_type=f32)
    readout = kept - removed * head_sum(erase_rate * q) + v * head_sum(repl * q)
    centered = readout - jnp.mean(readout, axis=-1, keepdims=True)
    variance = jnp.mean(centered * centered, axis=-1, keepdims=True)
    mixed = centered * lax.rsqrt(variance + group_eps) * gains(ag_ref)
    mixed_ref[...] = (mixed + head_sum(q * repl * gains(xg_ref)) * v).astype(bf16)
    high = removed.astype(bf16)
    low = (removed - high.astype(f32)).astype(bf16)
    both = jnp.concatenate([high, low], axis=1)
    rate_w, repl_w = wide(erase_rate), wide(repl)
    for c in range(chunks):
        part = pl.ds(c * width, width)
        gone = jnp.dot(both, spread_ref[:, part], preferred_element_type=f32)
        added = jnp.dot(v16, spread_ref[:span, part], preferred_element_type=f32)
        out_ref[:, part] = m_ref[:, part] * decay_w - gone * rate_w + added * repl_w


def update_state(q, k, v, decay_logit, rate_logit, gains, state):
    seqs, heads, cells = state.shape
    span = q.shape[1]
    block = 2 * heads
    row = pl.BlockSpec((block, span), lambda i: (i, 0))
    gain = pl.BlockSpec((heads, span), lambda i: (0, 0))
    big = pl.BlockSpec((block, cells), lambda i: (i, 0))
    mixed, new = pl.pallas_call(
        state_kernel,
        grid=(seqs * heads // block,),
        in_specs=[row] * 5 + [gain] * 4 + [big],
        out_specs=[row, big],
        out_shape=[
            jax.ShapeDtypeStruct((seqs * heads, span), jnp.bfloat16),
            jax.ShapeDtypeStruct((seqs * heads, cells), jnp.float32),
        ],
        scratch_shapes=[
            pltpu.VMEM((cells, span), jnp.bfloat16),
            pltpu.VMEM((2 * span, cells), jnp.bfloat16),
        ],
        compiler_params=pltpu.CompilerParams(vmem_limit_bytes=40 * 2**20),
        name="state",
    )(q, k, v, decay_logit, rate_logit, *gains, state.reshape(seqs * heads, cells))
    return mixed, new.reshape(state.shape)


def project_kernel(
    devices, x_ref, w_ref, out_ref, gathered, other, result, landed,
    x_send, x_recv, r_send, r_recv, w_send, w_recv, local_sem,
):
    me = lax.axis_index("ep")
    core, chip = me % 2, me // 2
    partner = me + 1 - 2 * core
    chips = devices // 2
    rows = x_ref.shape[0]
    barrier = pltpu.get_barrier_semaphore()
    pl.semaphore_signal(barrier, inc=1, device_id=(partner,), device_id_type=MESH)

    def greet(k, carry):
        pl.semaphore_signal(
            barrier, inc=1, device_id=((me + 2 * k) % devices,), device_id_type=MESH
        )
        return carry

    lax.fori_loop(1, chips, greet, 0)
    pl.semaphore_wait(barrier, chips)

    def token_copy(k):
        return pltpu.make_async_remote_copy(
            src_ref=x_ref,
            dst_ref=gathered.at[chip],
            send_sem=x_send.at[k],
            recv_sem=x_recv.at[k],
            device_id=((me + 2 * k) % devices,),
            device_id_type=MESH,
        )

    def result_copy(k):
        peer = (me + 2 * k) % devices
        return pltpu.make_async_remote_copy(
            src_ref=result.at[peer // 2],
            dst_ref=landed.at[chip],
            send_sem=r_send.at[k],
            recv_sem=r_recv.at[k],
            device_id=(peer,),
            device_id_type=MESH,
        )

    def start(make):
        def step(k, carry):
            make(k).start()
            return carry
        lax.fori_loop(1, chips, step, 0)

    def finish(make):
        def step(k, carry):
            make(k).wait()
            return carry
        lax.fori_loop(1, chips, step, 0)

    weights = pltpu.make_async_remote_copy(
        src_ref=w_ref,
        dst_ref=other,
        send_sem=w_send,
        recv_sem=w_recv,
        device_id=(partner,),
        device_id_type=MESH,
    )
    start(token_copy)
    weights.start()
    mine = pltpu.make_async_copy(x_ref, gathered.at[chip], local_sem)
    mine.start()
    mine.wait()
    weights.wait()
    finish(token_copy)
    tokens = gathered[...].reshape(chips * rows, x_ref.shape[1])
    for ref, at in ((w_ref, core), (other, 1 - core)):
        product = jnp.dot(tokens, ref[...], preferred_element_type=jnp.float32)
        product = product.astype(jnp.bfloat16)
        for c in range(chips):
            result[c, at] = product[c * rows : (c + 1) * rows]
    start(result_copy)
    mine = pltpu.make_async_copy(result.at[chip], landed.at[chip], local_sem)
    mine.start()
    mine.wait()
    finish(result_copy)
    out_ref[...] = landed[...]


def project(x, w, ident):
    devices = lax.axis_size("ep")
    chips = devices // 2
    rows, depth = x.shape
    columns = w.shape[1]
    shape = (chips, 2, rows, columns)
    out = pl.pallas_call(
        functools.partial(project_kernel, devices),
        out_shape=jax.ShapeDtypeStruct(shape, jnp.bfloat16),
        in_specs=[pl.BlockSpec(memory_space=pltpu.VMEM)] * 2,
        out_specs=pl.BlockSpec(memory_space=pltpu.VMEM),
        scratch_shapes=[
            pltpu.VMEM((chips, rows, depth), jnp.bfloat16),
            pltpu.VMEM(w.shape, jnp.bfloat16),
            pltpu.VMEM(shape, jnp.bfloat16),
            pltpu.VMEM(shape, jnp.bfloat16),
            pltpu.SemaphoreType.DMA((chips,)),
            pltpu.SemaphoreType.DMA((chips,)),
            pltpu.SemaphoreType.DMA((chips,)),
            pltpu.SemaphoreType.DMA((chips,)),
            pltpu.SemaphoreType.DMA,
            pltpu.SemaphoreType.DMA,
            pltpu.SemaphoreType.DMA,
        ],
        compiler_params=pltpu.CompilerParams(
            collective_id=ident, has_side_effects=True, vmem_limit_bytes=50 * 2**20
        ),
        name=f"project{ident}",
    )(x, w)
    return out.reshape(devices, rows, columns)


def exchange_kernel(devices, x_ref, out_ref, landed, send_sem, recv_sem, local_sem):
    me = lax.axis_index("ep")
    barrier = pltpu.get_barrier_semaphore()

    def greet(k, carry):
        pl.semaphore_signal(
            barrier, inc=1, device_id=((me + k) % devices,), device_id_type=MESH
        )
        return carry

    lax.fori_loop(1, devices, greet, 0)
    pl.semaphore_wait(barrier, devices - 1)

    def copy(k):
        peer = (me + k) % devices
        return pltpu.make_async_remote_copy(
            src_ref=x_ref.at[peer],
            dst_ref=landed.at[me],
            send_sem=send_sem.at[k],
            recv_sem=recv_sem.at[k],
            device_id=(peer,),
            device_id_type=MESH,
        )

    def start(k, carry):
        copy(k).start()
        return carry

    def finish(k, carry):
        copy(k).wait()
        return carry

    lax.fori_loop(1, devices, start, 0)
    mine = pltpu.make_async_copy(x_ref.at[me], landed.at[me], local_sem)
    mine.start()
    mine.wait()
    lax.fori_loop(1, devices, finish, 0)
    out_ref[...] = landed[...]


def exchange(x, ident):
    devices = lax.axis_size("ep")
    blocks = x.reshape(devices, -1, 128)
    out = pl.pallas_call(
        functools.partial(exchange_kernel, devices),
        out_shape=jax.ShapeDtypeStruct(blocks.shape, x.dtype),
        in_specs=[pl.BlockSpec(memory_space=pltpu.VMEM)],
        out_specs=pl.BlockSpec(memory_space=pltpu.VMEM),
        scratch_shapes=[
            pltpu.VMEM(blocks.shape, x.dtype),
            pltpu.SemaphoreType.DMA((devices,)),
            pltpu.SemaphoreType.DMA((devices,)),
            pltpu.SemaphoreType.DMA,
        ],
        compiler_params=pltpu.CompilerParams(collective_id=ident, has_side_effects=True),
        name=f"exchange{ident}",
    )(blocks)
    return out.reshape(x.shape)


def local(
    latest_embeddings,
    prior_memory_grids,
    earlier_rescale_gain,
    query_map,
    lookup_map,
    content_map,
    forget_lower_map,
    forget_upper_map,
    forget_shift,
    adapt_lower_map,
    adapt_upper_map,
    adapt_shift,
    erase_lookup_gains,
    substitute_lookup_gains,
    present_extra_gains,
    attender_rescale_gain,
    result_map,
    later_rescale_gain,
    specialist_switch_maps,
    specialist_widen_maps,
    specialist_shrink_maps,
    picked_specialists,
    specialist_picked_shares,
):
    seq_count, model_width = latest_embeddings.shape
    attender_count = prior_memory_grids.shape[1]
    channel_span = model_width // attender_count
    devices = lax.axis_size("ep")
    columns = query_map.shape[1]
    normed = rms_norm(latest_embeddings, earlier_rescale_gain)
    stacked = jnp.concatenate([query_map, lookup_map, content_map], axis=1)
    projected = project(normed, stacked, 0).reshape(devices, seq_count, 3, columns)
    projected = projected.transpose(2, 1, 0, 3).reshape(
        3, seq_count * attender_count, channel_span
    )
    decay_low = jnp.tanh(
        jnp.dot(normed, forget_lower_map, preferred_element_type=jnp.float32)
    ).astype(jnp.bfloat16)
    decay_logit = forget_shift + jnp.dot(
        decay_low, forget_upper_map, preferred_element_type=jnp.float32
    )
    rate_low = jnp.dot(normed, adapt_lower_map, preferred_element_type=jnp.float32).astype(
        jnp.bfloat16
    )
    rate_logit = adapt_shift + jnp.dot(
        rate_low, adapt_upper_map, preferred_element_type=jnp.float32
    )
    mixed, new_state = update_state(
        projected[0],
        projected[1],
        projected[2],
        decay_logit.reshape(-1, channel_span),
        rate_logit.reshape(-1, channel_span),
        [
            gain.reshape(attender_count, channel_span)
            for gain in (
                erase_lookup_gains,
                substitute_lookup_gains,
                present_extra_gains,
                attender_rescale_gain,
            )
        ],
        prior_memory_grids,
    )
    mixer_out = project(mixed.reshape(seq_count, model_width), result_map, 1)
    mixer_out = mixer_out.transpose(1, 0, 2).reshape(seq_count, model_width)
    residual = (latest_embeddings.astype(jnp.float32) + mixer_out.astype(jnp.float32)).astype(
        jnp.bfloat16
    )
    second = rms_norm(residual, later_rescale_gain)
    top_count = picked_specialists.shape[1]
    expert_count = specialist_switch_maps.shape[0] * devices
    group_size = expert_count // GROUPS
    capacity = ((seq_count + 1) // 2 * top_count + group_size - 1) // group_size
    flat_ids = picked_specialists.reshape(-1)
    matches = (flat_ids[:, None] == jnp.arange(expert_count, dtype=jnp.int32)[None, :]).astype(
        jnp.int32
    )
    slot_rank = jnp.sum((jnp.cumsum(matches, axis=0) - matches) * matches, axis=1)
    slot_ids = flat_ids * capacity + slot_rank
    picks = (
        slot_ids[:, None] == jnp.arange(expert_count * capacity, dtype=jnp.int32)[None, :]
    ).astype(jnp.bfloat16)
    repeated = jnp.repeat(second, top_count, axis=0)
    send_rows = jnp.einsum("sk,sd->kd", picks, repeated, preferred_element_type=jnp.float32).astype(
        jnp.bfloat16
    )
    send_rows = send_rows.reshape(devices, expert_count // devices * capacity, model_width)
    received = exchange(send_rows, 2)
    rows_in = received.reshape(-1, model_width)
    gate_proj = jnp.dot(rows_in, specialist_switch_maps[0], preferred_element_type=jnp.float32)
    up_proj = jnp.dot(rows_in, specialist_widen_maps[0], preferred_element_type=jnp.float32)
    hidden_act = (jax.nn.silu(gate_proj) * up_proj).astype(jnp.bfloat16)
    results = jnp.dot(
        hidden_act, specialist_shrink_maps[0], preferred_element_type=jnp.float32
    ).astype(jnp.bfloat16)
    returned = exchange(results.reshape(received.shape), 3)
    collected = jnp.dot(
        picks, returned.reshape(-1, model_width), preferred_element_type=jnp.float32
    )
    expert_sum = jnp.sum(
        collected.reshape(seq_count, top_count, model_width) * specialist_picked_shares[:, :, None],
        axis=1,
    )
    new_hidden = (residual.astype(jnp.float32) + expert_sum).astype(jnp.bfloat16)
    return (new_hidden, new_state)


def solution(mesh):
    return jax.shard_map(
        local,
        mesh=mesh,
        in_specs=(
            P("ep", None),
            P("ep", None, None),
            P(),
            P(None, "ep"),
            P(None, "ep"),
            P(None, "ep"),
            P(),
            P(),
            P(),
            P(),
            P(),
            P(),
            P(),
            P(),
            P(),
            P(),
            P(None, "ep"),
            P(),
            P("ep", None, None),
            P("ep", None, None),
            P("ep", None, None),
            P("ep", None),
            P("ep", None),
        ),
        out_specs=(P("ep", None), P("ep", None, None)),
        check_vma=False,
    )
```

```python
import functools
import math

import jax
import jax.numpy as jnp
from jax import lax
from jax.experimental import pallas as pl
from jax.experimental.pallas import tpu as pltpu
from jax.sharding import PartitionSpec as P

GROUPS = 4
MESH = pl.DeviceIdType.MESH
OUTER = 4

norm_eps = 1e-06
group_eps = 0.00064
unit_eps = 1e-06


def rms_norm(rows_in, gain):
    values = rows_in.astype(jnp.float32)
    scale = lax.rsqrt(jnp.mean(values * values, axis=-1, keepdims=True) + norm_eps)
    return (values * scale * gain).astype(jnp.bfloat16)


def state_kernel(
    q_ref, k_ref, v_ref, dl_ref, al_ref, eg_ref, sg_ref, xg_ref, ag_ref, m_ref,
    mixed_ref, out_ref, sum_ref, spread_ref,
):
    rows, span = q_ref.shape
    repeat = rows // eg_ref.shape[0]
    width = 4 * span
    chunks = m_ref.shape[1] // width
    f32, bf16 = jnp.float32, jnp.bfloat16

    @pl.when(pl.program_id(0) == 0)
    def _():
        shape = sum_ref.shape
        sum_ref[...] = jnp.where(
            lax.broadcasted_iota(jnp.int32, shape, 0) // span
            == lax.broadcasted_iota(jnp.int32, shape, 1),
            1.0, 0.0,
        ).astype(bf16)
        shape = spread_ref.shape
        spread_ref[...] = jnp.where(
            lax.broadcasted_iota(jnp.int32, shape, 1) // span
            == lax.broadcasted_iota(jnp.int32, shape, 0) % span,
            1.0, 0.0,
        ).astype(bf16)

    def gains(ref):
        return jnp.concatenate([ref[...]] * repeat, axis=0)

    def wide(x):
        return jnp.concatenate([x] * 4, axis=1)

    def head_sum(x):
        return jnp.sum(x, axis=-1, keepdims=True)

    q = q_ref[...].astype(f32)
    k = k_ref[...].astype(f32)
    v16 = v_ref[...]
    v = v16.astype(f32)
    decay = jnp.exp(-math.exp(-0.5) * jax.nn.sigmoid(dl_ref[...]))
    rate = jax.nn.sigmoid(al_ref[...])
    erase = k * gains(eg_ref)
    erase = erase * lax.rsqrt(head_sum(erase * erase) + unit_eps)
    repl = k * (1.0 + (rate - 1.0) * gains(sg_ref))
    erase_rate = erase * rate
    erase_w, decay_w, query_w = wide(erase), wide(decay), wide(decay * q)
    removed = jnp.zeros((rows, span), f32)
    kept = jnp.zeros((rows, span), f32)
    for c in range(chunks):
        part = pl.ds(c * width, width)
        m = m_ref[:, part]
        picker = sum_ref[part, :]
        removed += jnp.dot((m * erase_w).astype(bf16), picker, preferred_element_type=f32)
        kept += jnp.dot((m * query_w).astype(bf16), picker, preferred_element_type=f32)
    readout = kept - removed * head_sum(erase_rate * q) + v * head_sum(repl * q)
    centered = readout - jnp.mean(readout, axis=-1, keepdims=True)
    variance = jnp.mean(centered * centered, axis=-1, keepdims=True)
    mixed = centered * lax.rsqrt(variance + group_eps) * gains(ag_ref)
    mixed_ref[...] = (mixed + head_sum(q * repl * gains(xg_ref)) * v).astype(bf16)
    high = removed.astype(bf16)
    low = (removed - high.astype(f32)).astype(bf16)
    both = jnp.concatenate([high, low], axis=1)
    rate_w, repl_w = wide(erase_rate), wide(repl)
    for c in range(chunks):
        part = pl.ds(c * width, width)
        gone = jnp.dot(both, spread_ref[:, part], preferred_element_type=f32)
        added = jnp.dot(v16, spread_ref[:span, part], preferred_element_type=f32)
        out_ref[:, part] = m_ref[:, part] * decay_w - gone * rate_w + added * repl_w


def update_state(q, k, v, decay_logit, rate_logit, gains, state):
    seqs, heads, cells = state.shape
    span = q.shape[1]
    block = 2 * heads
    row = pl.BlockSpec((block, span), lambda i: (i, 0))
    gain = pl.BlockSpec((heads, span), lambda i: (0, 0))
    big = pl.BlockSpec((block, cells), lambda i: (i, 0))
    mixed, new = pl.pallas_call(
        state_kernel,
        grid=(seqs * heads // block,),
        in_specs=[row] * 5 + [gain] * 4 + [big],
        out_specs=[row, big],
        out_shape=[
            jax.ShapeDtypeStruct((seqs * heads, span), jnp.bfloat16),
            jax.ShapeDtypeStruct((seqs * heads, cells), jnp.float32),
        ],
        scratch_shapes=[
            pltpu.VMEM((cells, span), jnp.bfloat16),
            pltpu.VMEM((2 * span, cells), jnp.bfloat16),
        ],
        compiler_params=pltpu.CompilerParams(vmem_limit_bytes=16 * 2**20),
        name="state",
    )(q, k, v, decay_logit, rate_logit, *gains, state.reshape(seqs * heads, cells))
    return mixed, new.reshape(state.shape)


def project_kernel(
    devices, x_ref, w_ref, out_ref, gathered, other, result, landed,
    z_send, z_recv, x_send, x_recv, r_send, r_recv, w_send, w_recv, local_sem,
):
    me = lax.axis_index("ep")
    core, chip = me % 2, me // 2
    partner = me + 1 - 2 * core
    chips = devices // 2
    rows = x_ref.shape[0]
    barrier = pltpu.get_barrier_semaphore()
    pl.semaphore_signal(barrier, inc=1, device_id=(partner,), device_id_type=MESH)

    def greet(k, carry):
        pl.semaphore_signal(
            barrier, inc=1, device_id=((me + 2 * k) % devices,), device_id_type=MESH
        )
        return carry

    lax.fori_loop(1, chips, greet, 0)
    pl.semaphore_wait(barrier, chips)

    inner = chips // OUTER
    layer, place = chip // inner, chip % inner

    def block_of(j):
        return ((layer + OUTER - j) % OUTER) * inner + place

    def outer_copy(j):
        return pltpu.make_async_remote_copy(
            src_ref=x_ref,
            dst_ref=gathered.at[chip],
            send_sem=z_send.at[j],
            recv_sem=z_recv.at[j],
            device_id=((((layer + j) % OUTER) * inner + place) * 2 + core,),
            device_id_type=MESH,
        )

    def inner_copy(j, r):
        block = gathered.at[block_of(j)]
        return pltpu.make_async_remote_copy(
            src_ref=x_ref if j == 0 else block,
            dst_ref=block,
            send_sem=x_send.at[j, r],
            recv_sem=x_recv.at[j, r],
            device_id=((layer * inner + (place + r) % inner) * 2 + core,),
            device_id_type=MESH,
        )

    def inner_start(j):
        def step(r, carry):
            inner_copy(j, r).start()
            return carry
        lax.fori_loop(1, inner, step, 0)

    def inner_finish(j):
        def step(r, carry):
            inner_copy(j, r).wait()
            return carry
        lax.fori_loop(1, inner, step, 0)

    def result_copy(k):
        peer = (me + 2 * k) % devices
        return pltpu.make_async_remote_copy(
            src_ref=result.at[peer // 2],
            dst_ref=landed.at[chip],
            send_sem=r_send.at[k],
            recv_sem=r_recv.at[k],
            device_id=(peer,),
            device_id_type=MESH,
        )

    def start(make):
        def step(k, carry):
            make(k).start()
            return carry
        lax.fori_loop(1, chips, step, 0)

    def finish(make):
        def step(k, carry):
            make(k).wait()
            return carry
        lax.fori_loop(1, chips, step, 0)

    weights = pltpu.make_async_remote_copy(
        src_ref=w_ref,
        dst_ref=other,
        send_sem=w_send,
        recv_sem=w_recv,
        device_id=(partner,),
        device_id_type=MESH,
    )
    for j in range(1, OUTER):
        outer_copy(j).start()
    inner_start(0)
    weights.start()
    mine = pltpu.make_async_copy(x_ref, gathered.at[chip], local_sem)
    mine.start()
    mine.wait()
    for j in range(1, OUTER):
        outer_copy(j).wait_recv()
        inner_start(j)
    weights.wait()
    for j in range(1, OUTER):
        outer_copy(j).wait_send()
    for j in range(OUTER):
        inner_finish(j)
    tokens = gathered[...].reshape(chips * rows, x_ref.shape[1])
    for ref, at in ((w_ref, core), (other, 1 - core)):
        product = lax.dot_general(
            tokens, ref[...], (((1,), (1,)), ((), ())), preferred_element_type=jnp.float32
        )
        product = product.astype(jnp.bfloat16)
        for c in range(chips):
            result[c, at] = product[c * rows : (c + 1) * rows]
    start(result_copy)
    mine = pltpu.make_async_copy(result.at[chip], landed.at[chip], local_sem)
    mine.start()
    mine.wait()
    finish(result_copy)
    out_ref[...] = landed[...]


def project(x, w, ident):
    devices = lax.axis_size("ep")
    chips = devices // 2
    rows, depth = x.shape
    columns = w.shape[0]
    shape = (chips, 2, rows, columns)
    out = pl.pallas_call(
        functools.partial(project_kernel, devices),
        out_shape=jax.ShapeDtypeStruct(shape, jnp.bfloat16),
        in_specs=[pl.BlockSpec(memory_space=pltpu.VMEM)] * 2,
        out_specs=pl.BlockSpec(memory_space=pltpu.VMEM),
        scratch_shapes=[
            pltpu.VMEM((chips, rows, depth), jnp.bfloat16),
            pltpu.VMEM(w.shape, jnp.bfloat16),
            pltpu.VMEM(shape, jnp.bfloat16),
            pltpu.VMEM(shape, jnp.bfloat16),
            pltpu.SemaphoreType.DMA((OUTER,)),
            pltpu.SemaphoreType.DMA((OUTER,)),
            pltpu.SemaphoreType.DMA((OUTER, chips // OUTER)),
            pltpu.SemaphoreType.DMA((OUTER, chips // OUTER)),
            pltpu.SemaphoreType.DMA((chips,)),
            pltpu.SemaphoreType.DMA((chips,)),
            pltpu.SemaphoreType.DMA,
            pltpu.SemaphoreType.DMA,
            pltpu.SemaphoreType.DMA,
        ],
        compiler_params=pltpu.CompilerParams(
            collective_id=ident, has_side_effects=True, vmem_limit_bytes=20 * 2**20
        ),
        cost_estimate=pl.CostEstimate(
            flops=4 * chips * rows * depth * columns,
            bytes_accessed=32 * chips * rows * depth * 2,
            transcendentals=0,
        ),
        name=f"project{ident}",
    )(x, w)
    return out.reshape(devices, rows, columns)


def exchange_kernel(devices, x_ref, out_ref, landed, send_sem, recv_sem, local_sem):
    me = lax.axis_index("ep")
    barrier = pltpu.get_barrier_semaphore()

    def greet(k, carry):
        pl.semaphore_signal(
            barrier, inc=1, device_id=((me + k) % devices,), device_id_type=MESH
        )
        return carry

    lax.fori_loop(1, devices, greet, 0)
    pl.semaphore_wait(barrier, devices - 1)

    def copy(k):
        peer = (me + k) % devices
        return pltpu.make_async_remote_copy(
            src_ref=x_ref.at[peer],
            dst_ref=landed.at[me],
            send_sem=send_sem.at[k],
            recv_sem=recv_sem.at[k],
            device_id=(peer,),
            device_id_type=MESH,
        )

    def start(k, carry):
        copy(k).start()
        return carry

    def finish(k, carry):
        copy(k).wait()
        return carry

    lax.fori_loop(1, devices, start, 0)
    mine = pltpu.make_async_copy(x_ref.at[me], landed.at[me], local_sem)
    mine.start()
    mine.wait()
    lax.fori_loop(1, devices, finish, 0)
    out_ref[...] = landed[...]


def exchange(x, ident):
    devices = lax.axis_size("ep")
    blocks = x.reshape(devices, -1, 128)
    out = pl.pallas_call(
        functools.partial(exchange_kernel, devices),
        out_shape=jax.ShapeDtypeStruct(blocks.shape, x.dtype),
        in_specs=[pl.BlockSpec(memory_space=pltpu.VMEM)],
        out_specs=pl.BlockSpec(memory_space=pltpu.VMEM),
        scratch_shapes=[
            pltpu.VMEM(blocks.shape, x.dtype),
            pltpu.SemaphoreType.DMA((devices,)),
            pltpu.SemaphoreType.DMA((devices,)),
            pltpu.SemaphoreType.DMA,
        ],
        compiler_params=pltpu.CompilerParams(collective_id=ident, has_side_effects=True),
        name=f"exchange{ident}",
    )(blocks)
    return out.reshape(x.shape)


def local(
    latest_embeddings,
    prior_memory_grids,
    earlier_rescale_gain,
    query_map,
    lookup_map,
    content_map,
    forget_lower_map,
    forget_upper_map,
    forget_shift,
    adapt_lower_map,
    adapt_upper_map,
    adapt_shift,
    erase_lookup_gains,
    substitute_lookup_gains,
    present_extra_gains,
    attender_rescale_gain,
    result_map,
    later_rescale_gain,
    specialist_switch_maps,
    specialist_widen_maps,
    specialist_shrink_maps,
    picked_specialists,
    specialist_picked_shares,
):
    seq_count, model_width = latest_embeddings.shape
    attender_count = prior_memory_grids.shape[1]
    channel_span = model_width // attender_count
    devices = lax.axis_size("ep")
    columns = query_map.shape[1]
    normed = rms_norm(latest_embeddings, earlier_rescale_gain)
    stacked = jnp.concatenate([query_map.T, lookup_map.T, content_map.T], axis=0)
    projected = project(normed, stacked, 0).reshape(devices, seq_count, 3, columns)
    projected = projected.transpose(2, 1, 0, 3).reshape(
        3, seq_count * attender_count, channel_span
    )
    decay_low = jnp.tanh(
        jnp.dot(normed, forget_lower_map, preferred_element_type=jnp.float32)
    ).astype(jnp.bfloat16)
    decay_logit = forget_shift + jnp.dot(
        decay_low, forget_upper_map, preferred_element_type=jnp.float32
    )
    rate_low = jnp.dot(normed, adapt_lower_map, preferred_element_type=jnp.float32).astype(
        jnp.bfloat16
    )
    rate_logit = adapt_shift + jnp.dot(
        rate_low, adapt_upper_map, preferred_element_type=jnp.float32
    )
    mixed, new_state = update_state(
        projected[0],
        projected[1],
        projected[2],
        decay_logit.reshape(-1, channel_span),
        rate_logit.reshape(-1, channel_span),
        [
            gain.reshape(attender_count, channel_span)
            for gain in (
                erase_lookup_gains,
                substitute_lookup_gains,
                present_extra_gains,
                attender_rescale_gain,
            )
        ],
        prior_memory_grids,
    )
    mixer_out = project(mixed.reshape(seq_count, model_width), result_map.T, 1)
    mixer_out = mixer_out.transpose(1, 0, 2).reshape(seq_count, model_width)
    residual = (latest_embeddings.astype(jnp.float32) + mixer_out.astype(jnp.float32)).astype(
        jnp.bfloat16
    )
    second = rms_norm(residual, later_rescale_gain)
    top_count = picked_specialists.shape[1]
    expert_count = specialist_switch_maps.shape[0] * devices
    group_size = expert_count // GROUPS
    capacity = ((seq_count + 1) // 2 * top_count + group_size - 1) // group_size
    flat_ids = picked_specialists.reshape(-1)
    matches = (flat_ids[:, None] == jnp.arange(expert_count, dtype=jnp.int32)[None, :]).astype(
        jnp.int32
    )
    slot_rank = jnp.sum((jnp.cumsum(matches, axis=0) - matches) * matches, axis=1)
    slot_ids = flat_ids * capacity + slot_rank
    picks = (
        slot_ids[:, None] == jnp.arange(expert_count * capacity, dtype=jnp.int32)[None, :]
    ).astype(jnp.bfloat16)
    repeated = jnp.repeat(second, top_count, axis=0)
    send_rows = jnp.einsum("sk,sd->kd", picks, repeated, preferred_element_type=jnp.float32).astype(
        jnp.bfloat16
    )
    send_rows = send_rows.reshape(devices, expert_count // devices * capacity, model_width)
    received = exchange(send_rows, 2)
    rows_in = received.reshape(-1, model_width)
    gate_proj = jnp.dot(rows_in, specialist_switch_maps[0], preferred_element_type=jnp.float32)
    up_proj = jnp.dot(rows_in, specialist_widen_maps[0], preferred_element_type=jnp.float32)
    hidden_act = (jax.nn.silu(gate_proj) * up_proj).astype(jnp.bfloat16)
    results = jnp.dot(
        hidden_act, specialist_shrink_maps[0], preferred_element_type=jnp.float32
    ).astype(jnp.bfloat16)
    returned = exchange(results.reshape(received.shape), 3)
    collected = jnp.dot(
        picks, returned.reshape(-1, model_width), preferred_element_type=jnp.float32
    )
    expert_sum = jnp.sum(
        collected.reshape(seq_count, top_count, model_width) * specialist_picked_shares[:, :, None],
        axis=1,
    )
    new_hidden = (residual.astype(jnp.float32) + expert_sum).astype(jnp.bfloat16)
    return (new_hidden, new_state)


def solution(mesh):
    return jax.shard_map(
        local,
        mesh=mesh,
        in_specs=(
            P("ep", None),
            P("ep", None, None),
            P(),
            P(None, "ep"),
            P(None, "ep"),
            P(None, "ep"),
            P(),
            P(),
            P(),
            P(),
            P(),
            P(),
            P(),
            P(),
            P(),
            P(),
            P(None, "ep"),
            P(),
            P("ep", None, None),
            P("ep", None, None),
            P("ep", None, None),
            P("ep", None),
            P("ep", None),
        ),
        out_specs=(P("ep", None), P("ep", None, None)),
        check_vma=False,
    )
```

```python
import functools
import math

import jax
import jax.numpy as jnp
from jax import lax
from jax.experimental import pallas as pl
from jax.experimental.pallas import tpu as pltpu
from jax.sharding import PartitionSpec as P

GROUPS = 4
MESH = pl.DeviceIdType.MESH
OUTER = 4

norm_eps = 1e-06
group_eps = 0.00064
unit_eps = 1e-06


def rms_norm(rows_in, gain):
    values = rows_in.astype(jnp.float32)
    scale = lax.rsqrt(jnp.mean(values * values, axis=-1, keepdims=True) + norm_eps)
    return (values * scale * gain).astype(jnp.bfloat16)


def state_kernel(
    q_ref, k_ref, v_ref, dl_ref, al_ref, eg_ref, sg_ref, xg_ref, ag_ref, m_ref,
    mixed_ref, out_ref, sum_ref, spread_ref,
):
    rows, span = q_ref.shape
    repeat = rows // eg_ref.shape[0]
    width = 4 * span
    chunks = m_ref.shape[1] // width
    f32, bf16 = jnp.float32, jnp.bfloat16

    @pl.when(pl.program_id(0) == 0)
    def _():
        shape = sum_ref.shape
        sum_ref[...] = jnp.where(
            lax.broadcasted_iota(jnp.int32, shape, 0) // span
            == lax.broadcasted_iota(jnp.int32, shape, 1),
            1.0, 0.0,
        ).astype(bf16)
        shape = spread_ref.shape
        spread_ref[...] = jnp.where(
            lax.broadcasted_iota(jnp.int32, shape, 1) // span
            == lax.broadcasted_iota(jnp.int32, shape, 0) % span,
            1.0, 0.0,
        ).astype(bf16)

    def gains(ref):
        return jnp.concatenate([ref[...]] * repeat, axis=0)

    def wide(x):
        return jnp.concatenate([x] * 4, axis=1)

    def head_sum(x):
        return jnp.sum(x, axis=-1, keepdims=True)

    q = q_ref[...].astype(f32)
    k = k_ref[...].astype(f32)
    v16 = v_ref[...]
    v = v16.astype(f32)
    decay = jnp.exp(-math.exp(-0.5) * jax.nn.sigmoid(dl_ref[...]))
    rate = jax.nn.sigmoid(al_ref[...])
    erase = k * gains(eg_ref)
    erase = erase * lax.rsqrt(head_sum(erase * erase) + unit_eps)
    repl = k * (1.0 + (rate - 1.0) * gains(sg_ref))
    erase_rate = erase * rate
    erase_w, decay_w, query_w = wide(erase), wide(decay), wide(decay * q)
    removed = jnp.zeros((rows, span), f32)
    kept = jnp.zeros((rows, span), f32)
    for c in range(chunks):
        part = pl.ds(c * width, width)
        m = m_ref[:, part]
        picker = sum_ref[part, :]
        removed += jnp.dot((m * erase_w).astype(bf16), picker, preferred_element_type=f32)
        kept += jnp.dot((m * query_w).astype(bf16), picker, preferred_element_type=f32)
    readout = kept - removed * head_sum(erase_rate * q) + v * head_sum(repl * q)
    centered = readout - jnp.mean(readout, axis=-1, keepdims=True)
    variance = jnp.mean(centered * centered, axis=-1, keepdims=True)
    mixed = centered * lax.rsqrt(variance + group_eps) * gains(ag_ref)
    mixed_ref[...] = (mixed + head_sum(q * repl * gains(xg_ref)) * v).astype(bf16)
    high = removed.astype(bf16)
    low = (removed - high.astype(f32)).astype(bf16)
    both = jnp.concatenate([high, low], axis=1)
    rate_w, repl_w = wide(erase_rate), wide(repl)
    for c in range(chunks):
        part = pl.ds(c * width, width)
        gone = jnp.dot(both, spread_ref[:, part], preferred_element_type=f32)
        added = jnp.dot(v16, spread_ref[:span, part], preferred_element_type=f32)
        out_ref[:, part] = m_ref[:, part] * decay_w - gone * rate_w + added * repl_w


def update_state(q, k, v, decay_logit, rate_logit, gains, state):
    seqs, heads, cells = state.shape
    span = q.shape[1]
    block = 2 * heads
    row = pl.BlockSpec((block, span), lambda i: (i, 0))
    gain = pl.BlockSpec((heads, span), lambda i: (0, 0))
    big = pl.BlockSpec((block, cells), lambda i: (i, 0))
    mixed, new = pl.pallas_call(
        state_kernel,
        grid=(seqs * heads // block,),
        in_specs=[row] * 5 + [gain] * 4 + [big],
        out_specs=[row, big],
        out_shape=[
            jax.ShapeDtypeStruct((seqs * heads, span), jnp.bfloat16),
            jax.ShapeDtypeStruct((seqs * heads, cells), jnp.float32),
        ],
        scratch_shapes=[
            pltpu.VMEM((cells, span), jnp.bfloat16),
            pltpu.VMEM((2 * span, cells), jnp.bfloat16),
        ],
        compiler_params=pltpu.CompilerParams(vmem_limit_bytes=16 * 2**20),
        name="state",
    )(q, k, v, decay_logit, rate_logit, *gains, state.reshape(seqs * heads, cells))
    return mixed, new.reshape(state.shape)


def project_kernel(
    devices, x_ref, w_ref, out_ref, gathered, other, result, landed,
    z_send, z_recv, x_send, x_recv, r_send, r_recv, w_send, w_recv, local_sem,
):
    me = lax.axis_index("ep")
    core, chip = me % 2, me // 2
    partner = me + 1 - 2 * core
    chips = devices // 2
    rows = x_ref.shape[0]
    barrier = pltpu.get_barrier_semaphore()
    pl.semaphore_signal(barrier, inc=1, device_id=(partner,), device_id_type=MESH)

    def greet(k, carry):
        pl.semaphore_signal(
            barrier, inc=1, device_id=((me + 2 * k) % devices,), device_id_type=MESH
        )
        return carry

    lax.fori_loop(1, chips, greet, 0)
    pl.semaphore_wait(barrier, chips)

    inner = chips // OUTER
    layer, place = chip // inner, chip % inner

    def block_of(j):
        return ((layer + OUTER - j) % OUTER) * inner + place

    def outer_copy(j):
        return pltpu.make_async_remote_copy(
            src_ref=x_ref,
            dst_ref=gathered.at[chip],
            send_sem=z_send.at[j],
            recv_sem=z_recv.at[j],
            device_id=((((layer + j) % OUTER) * inner + place) * 2 + core,),
            device_id_type=MESH,
        )

    def inner_copy(j, r):
        block = gathered.at[block_of(j)]
        return pltpu.make_async_remote_copy(
            src_ref=x_ref if j == 0 else block,
            dst_ref=block,
            send_sem=x_send.at[j, r],
            recv_sem=x_recv.at[j, r],
            device_id=((layer * inner + (place + r) % inner) * 2 + core,),
            device_id_type=MESH,
        )

    def inner_start(j):
        def step(r, carry):
            inner_copy(j, r).start()
            return carry
        lax.fori_loop(1, inner, step, 0)

    def inner_finish(j):
        def step(r, carry):
            inner_copy(j, r).wait()
            return carry
        lax.fori_loop(1, inner, step, 0)

    def result_copy(k):
        peer = (me + 2 * k) % devices
        return pltpu.make_async_remote_copy(
            src_ref=result.at[peer // 2],
            dst_ref=landed.at[chip],
            send_sem=r_send.at[k],
            recv_sem=r_recv.at[k],
            device_id=(peer,),
            device_id_type=MESH,
        )

    def start(make):
        def step(k, carry):
            make(k).start()
            return carry
        lax.fori_loop(1, chips, step, 0)

    def finish(make):
        def step(k, carry):
            make(k).wait()
            return carry
        lax.fori_loop(1, chips, step, 0)

    weights = pltpu.make_async_remote_copy(
        src_ref=w_ref,
        dst_ref=other,
        send_sem=w_send,
        recv_sem=w_recv,
        device_id=(partner,),
        device_id_type=MESH,
    )
    for j in range(1, OUTER):
        outer_copy(j).start()
    inner_start(0)
    weights.start()
    mine = pltpu.make_async_copy(x_ref, gathered.at[chip], local_sem)
    mine.start()
    mine.wait()
    for j in range(1, OUTER):
        outer_copy(j).wait_recv()
        inner_start(j)
    weights.wait()
    for j in range(1, OUTER):
        outer_copy(j).wait_send()
    for j in range(OUTER):
        inner_finish(j)
        base = ((layer + OUTER - j) % OUTER) * inner
        tokens = gathered[pl.ds(base, inner)].reshape(inner * rows, x_ref.shape[1])
        for ref, at in ((w_ref, core), (other, 1 - core)):
            product = lax.dot_general(
                tokens, ref[...], (((1,), (1,)), ((), ())), preferred_element_type=jnp.float32
            )
            product = product.astype(jnp.bfloat16)
            for c in range(inner):
                result[base + c, at] = product[c * rows : (c + 1) * rows]
    start(result_copy)
    mine = pltpu.make_async_copy(result.at[chip], landed.at[chip], local_sem)
    mine.start()
    mine.wait()
    finish(result_copy)
    out_ref[...] = landed[...]


def project(x, w, ident):
    devices = lax.axis_size("ep")
    chips = devices // 2
    rows, depth = x.shape
    columns = w.shape[0]
    shape = (chips, 2, rows, columns)
    out = pl.pallas_call(
        functools.partial(project_kernel, devices),
        out_shape=jax.ShapeDtypeStruct(shape, jnp.bfloat16),
        in_specs=[pl.BlockSpec(memory_space=pltpu.VMEM)] * 2,
        out_specs=pl.BlockSpec(memory_space=pltpu.VMEM),
        scratch_shapes=[
            pltpu.VMEM((chips, rows, depth), jnp.bfloat16),
            pltpu.VMEM(w.shape, jnp.bfloat16),
            pltpu.VMEM(shape, jnp.bfloat16),
            pltpu.VMEM(shape, jnp.bfloat16),
            pltpu.SemaphoreType.DMA((OUTER,)),
            pltpu.SemaphoreType.DMA((OUTER,)),
            pltpu.SemaphoreType.DMA((OUTER, chips // OUTER)),
            pltpu.SemaphoreType.DMA((OUTER, chips // OUTER)),
            pltpu.SemaphoreType.DMA((chips,)),
            pltpu.SemaphoreType.DMA((chips,)),
            pltpu.SemaphoreType.DMA,
            pltpu.SemaphoreType.DMA,
            pltpu.SemaphoreType.DMA,
        ],
        compiler_params=pltpu.CompilerParams(
            collective_id=ident, has_side_effects=True, vmem_limit_bytes=20 * 2**20
        ),
        cost_estimate=pl.CostEstimate(
            flops=4 * chips * rows * depth * columns,
            bytes_accessed=32 * chips * rows * depth * 2,
            transcendentals=0,
        ),
        name=f"project{ident}",
    )(x, w)
    return out.reshape(devices, rows, columns)


def exchange_kernel(devices, x_ref, out_ref, landed, send_sem, recv_sem, local_sem):
    me = lax.axis_index("ep")
    barrier = pltpu.get_barrier_semaphore()

    def greet(k, carry):
        pl.semaphore_signal(
            barrier, inc=1, device_id=((me + k) % devices,), device_id_type=MESH
        )
        return carry

    lax.fori_loop(1, devices, greet, 0)
    pl.semaphore_wait(barrier, devices - 1)

    def copy(k):
        peer = (me + k) % devices
        return pltpu.make_async_remote_copy(
            src_ref=x_ref.at[peer],
            dst_ref=landed.at[me],
            send_sem=send_sem.at[k],
            recv_sem=recv_sem.at[k],
            device_id=(peer,),
            device_id_type=MESH,
        )

    def start(k, carry):
        copy(k).start()
        return carry

    def finish(k, carry):
        copy(k).wait()
        return carry

    lax.fori_loop(1, devices, start, 0)
    mine = pltpu.make_async_copy(x_ref.at[me], landed.at[me], local_sem)
    mine.start()
    mine.wait()
    lax.fori_loop(1, devices, finish, 0)
    out_ref[...] = landed[...]


def exchange(x, ident):
    devices = lax.axis_size("ep")
    blocks = x.reshape(devices, -1, 128)
    out = pl.pallas_call(
        functools.partial(exchange_kernel, devices),
        out_shape=jax.ShapeDtypeStruct(blocks.shape, x.dtype),
        in_specs=[pl.BlockSpec(memory_space=pltpu.VMEM)],
        out_specs=pl.BlockSpec(memory_space=pltpu.VMEM),
        scratch_shapes=[
            pltpu.VMEM(blocks.shape, x.dtype),
            pltpu.SemaphoreType.DMA((devices,)),
            pltpu.SemaphoreType.DMA((devices,)),
            pltpu.SemaphoreType.DMA,
        ],
        compiler_params=pltpu.CompilerParams(collective_id=ident, has_side_effects=True),
        name=f"exchange{ident}",
    )(blocks)
    return out.reshape(x.shape)


def local(
    latest_embeddings,
    prior_memory_grids,
    earlier_rescale_gain,
    query_map,
    lookup_map,
    content_map,
    forget_lower_map,
    forget_upper_map,
    forget_shift,
    adapt_lower_map,
    adapt_upper_map,
    adapt_shift,
    erase_lookup_gains,
    substitute_lookup_gains,
    present_extra_gains,
    attender_rescale_gain,
    result_map,
    later_rescale_gain,
    specialist_switch_maps,
    specialist_widen_maps,
    specialist_shrink_maps,
    picked_specialists,
    specialist_picked_shares,
):
    seq_count, model_width = latest_embeddings.shape
    attender_count = prior_memory_grids.shape[1]
    channel_span = model_width // attender_count
    devices = lax.axis_size("ep")
    columns = query_map.shape[1]
    normed = rms_norm(latest_embeddings, earlier_rescale_gain)
    stacked = jnp.concatenate([query_map.T, lookup_map.T, content_map.T], axis=0)
    projected = project(normed, stacked, 0).reshape(devices, seq_count, 3, columns)
    projected = projected.transpose(2, 1, 0, 3).reshape(
        3, seq_count * attender_count, channel_span
    )
    decay_low = jnp.tanh(
        jnp.dot(normed, forget_lower_map, preferred_element_type=jnp.float32)
    ).astype(jnp.bfloat16)
    decay_logit = forget_shift + jnp.dot(
        decay_low, forget_upper_map, preferred_element_type=jnp.float32
    )
    rate_low = jnp.dot(normed, adapt_lower_map, preferred_element_type=jnp.float32).astype(
        jnp.bfloat16
    )
    rate_logit = adapt_shift + jnp.dot(
        rate_low, adapt_upper_map, preferred_element_type=jnp.float32
    )
    mixed, new_state = update_state(
        projected[0],
        projected[1],
        projected[2],
        decay_logit.reshape(-1, channel_span),
        rate_logit.reshape(-1, channel_span),
        [
            gain.reshape(attender_count, channel_span)
            for gain in (
                erase_lookup_gains,
                substitute_lookup_gains,
                present_extra_gains,
                attender_rescale_gain,
            )
        ],
        prior_memory_grids,
    )
    mixer_out = project(mixed.reshape(seq_count, model_width), result_map.T, 1)
    mixer_out = mixer_out.transpose(1, 0, 2).reshape(seq_count, model_width)
    residual = (latest_embeddings.astype(jnp.float32) + mixer_out.astype(jnp.float32)).astype(
        jnp.bfloat16
    )
    second = rms_norm(residual, later_rescale_gain)
    top_count = picked_specialists.shape[1]
    expert_count = specialist_switch_maps.shape[0] * devices
    group_size = expert_count // GROUPS
    capacity = ((seq_count + 1) // 2 * top_count + group_size - 1) // group_size
    flat_ids = picked_specialists.reshape(-1)
    matches = (flat_ids[:, None] == jnp.arange(expert_count, dtype=jnp.int32)[None, :]).astype(
        jnp.int32
    )
    slot_rank = jnp.sum((jnp.cumsum(matches, axis=0) - matches) * matches, axis=1)
    slot_ids = flat_ids * capacity + slot_rank
    picks = (
        slot_ids[:, None] == jnp.arange(expert_count * capacity, dtype=jnp.int32)[None, :]
    ).astype(jnp.bfloat16)
    repeated = jnp.repeat(second, top_count, axis=0)
    send_rows = jnp.einsum("sk,sd->kd", picks, repeated, preferred_element_type=jnp.float32).astype(
        jnp.bfloat16
    )
    send_rows = send_rows.reshape(devices, expert_count // devices * capacity, model_width)
    received = exchange(send_rows, 2)
    rows_in = received.reshape(-1, model_width)
    gate_proj = jnp.dot(rows_in, specialist_switch_maps[0], preferred_element_type=jnp.float32)
    up_proj = jnp.dot(rows_in, specialist_widen_maps[0], preferred_element_type=jnp.float32)
    hidden_act = (jax.nn.silu(gate_proj) * up_proj).astype(jnp.bfloat16)
    results = jnp.dot(
        hidden_act, specialist_shrink_maps[0], preferred_element_type=jnp.float32
    ).astype(jnp.bfloat16)
    returned = exchange(results.reshape(received.shape), 3)
    collected = jnp.dot(
        picks, returned.reshape(-1, model_width), preferred_element_type=jnp.float32
    )
    expert_sum = jnp.sum(
        collected.reshape(seq_count, top_count, model_width) * specialist_picked_shares[:, :, None],
        axis=1,
    )
    new_hidden = (residual.astype(jnp.float32) + expert_sum).astype(jnp.bfloat16)
    return (new_hidden, new_state)


def solution(mesh):
    return jax.shard_map(
        local,
        mesh=mesh,
        in_specs=(
            P("ep", None),
            P("ep", None, None),
            P(),
            P(None, "ep"),
            P(None, "ep"),
            P(None, "ep"),
            P(),
            P(),
            P(),
            P(),
            P(),
            P(),
            P(),
            P(),
            P(),
            P(),
            P(None, "ep"),
            P(),
            P("ep", None, None),
            P("ep", None, None),
            P("ep", None, None),
            P("ep", None),
            P("ep", None),
        ),
        out_specs=(P("ep", None), P("ep", None, None)),
        check_vma=False,
    )
```
